256 devices in a mesh: sp: 16 (over y, x), tp: 16 (over z, core).
Axes of the slice: x: 4, y: 4, z: 8, core: 2. Of those that a mesh axis runs over, the one named last changes fastest.
Arguments:
- queries: bfloat16 [16384, 2048], P('sp', 'tp'), may hold values from -8 to 8
- keys: bfloat16 [16384, 1024], P('sp', 'tp'), may hold values from -8 to 8
- values: bfloat16 [16384, 1024], P('sp', 'tp'), may hold values from -6 to 6
- doc_ids: int32 [16384], P('sp'), may hold values from 0 to 7, never falling along the last dimension, each value on 1 to 3072 neighbouring positions
- sink_logits: float32 [32], P('tp'), may hold values from 3 to 6
- out_weight: bfloat16 [2048, 2048], P('tp'), may hold values from -0.75 to 0.75
- residual: bfloat16 [16384, 2048], P(('sp', 'tp')), may hold values from -6 to 6
- norm_gain: float32 [2048], replicated, may hold values from 0.1 to 1.9
- routes: int32 [16384, 2], P(('sp', 'tp')), may hold values from 0 to 15, all different within a row; in each aligned block of 64 rows (0 to 63, 64 to 127, ...) at most 9 rows name the same one
- route_weights: float32 [16384, 2], P(('sp', 'tp')), may hold values from 0.2 to 1
- gate_weight: bfloat16 [16, 2048, 7168], P('sp', None, 'tp'), may hold values from -0.125 to 0.125
- up_weight: bfloat16 [16, 2048, 7168], P('sp', None, 'tp'), may hold values from -0.125 to 0.125
- down_weight: bfloat16 [16, 7168, 2048], P('sp', 'tp'), may hold values from -0.0625 to 0.0625
Outputs:
- layer_output: bfloat16 [16384, 2048], P(('sp', 'tp'))
The draws below stay inside these ranges and needn't reach their ends.
Inputs may be any that keep to these rules, and one draw needn't show every extreme that they name: `doc_ids`: never falling along the sequence; each document spans 1 to 3072 positions, one exactly that many. `routes`: each row names 2 different experts. In the rows of one device (aligned blocks of 64 rows) no expert is named by more than 9 rows, a bound that some block reaches.
All inputs are finite; a program needn't handle non-finite values.
Results may differ from the reference program's by a relative error of at most 0.015.
Values may be sent and summed in bfloat16 or wider, within the bound.
A program may use at most 128 MiB of HBM per device.

```python
import math
import jax
import jax.numpy as jnp
import numpy as np
from jax import lax

D = 2048
HEADS = 32
KV_HEADS = 16
HEAD_DIM = 64
WINDOW = 128
FF = 7168
TOP_K = 2
TOK_DEV = 64
TOK_SP = 1024
SEQ = 16384
EXPERTS = 16
CAP = 9
DOCS = 8
N_TP = 16


def draw_queries(key, part):
    normal_values = jnp.clip(jax.random.normal(jax.random.fold_in(key, 1), (SEQ, HEADS * HEAD_DIM), jnp.float32), -6.0, 6.0)
    return normal_values.astype(jnp.bfloat16)


def draw_keys(key, part):
    normal_values = jnp.clip(jax.random.normal(jax.random.fold_in(key, 2), (SEQ, KV_HEADS * HEAD_DIM), jnp.float32), -6.0, 6.0)
    return normal_values.astype(jnp.bfloat16)


def block_scale(rng, dims, cuts, smallest, top_value):
    level = 1.0
    for axis_at, parts in cuts:
        heights = jax.random.uniform(jax.random.fold_in(jax.random.fold_in(rng, 6), axis_at), (parts,), jnp.float32, smallest / len(cuts), top_value / len(cuts))
        level = level * jnp.repeat(jnp.exp(heights), dims[axis_at] // parts).reshape((-1,) + (1,) * (len(dims) - 1 - axis_at))
    return level


def length_profile(amount, total, limit, skew):
    portions = [(1 << 20) // math.isqrt(grade ** skew) + 1 for grade in range(2, amount + 1)]
    surplus, given = total - limit - (amount - 1), [1] * (amount - 1)
    while surplus > 0:
        movable = [i for i in range(amount - 1) if given[i] < limit]
        mass, remaining = sum([portions[i] for i in movable]), surplus
        for i in movable:
            more = min(limit - given[i], max(1, remaining * portions[i] // mass), surplus)
            given[i] = given[i] + more
            surplus = surplus - more
    return np.array([limit] + given)


def ragged_sizes(stream_key, number_of, total, most, skew):
    if number_of == 2:
        one = jax.random.randint(stream_key, (), max(1, total - most), min(most, total - 1) + 1)
        return jnp.stack([one, total - one])
    lengths = jnp.asarray(length_profile(number_of, total, most, skew), jnp.int32)
    twos = (number_of - 1) // 2
    donor, sink = lengths[1:1 + 2 * twos:2], lengths[2:2 + 2 * twos:2]
    slack = jnp.minimum(donor - 1, most - sink)
    passed = jax.random.randint(jax.random.fold_in(stream_key, 1), (twos,), 0, 1 << 20) % (slack + 1)
    lengths = lengths.at[1:1 + 2 * twos:2].set(donor - passed).at[2:2 + 2 * twos:2].set(sink + passed)
    return lengths[jax.random.permutation(jax.random.fold_in(stream_key, 2), number_of)]


def deal_out(own_key, own, number, rows, number_of, top, reach, lean):
    order = jax.random.permutation(own_key, number_of)
    heavy_load, ordinary = load_shares(number_of, rows * top, reach, lean, True), load_shares(number_of, rows * top, reach, lean, False)
    places = jnp.arange(number_of)

    def named(sizes, turn):
        used = int((sizes > 0).sum())
        fixed = max(1, used // 4)
        passed = fixed + (places - fixed + turn * (used - fixed)) % max(1, number_of - fixed)
        return jnp.zeros((number_of,), jnp.int32).at[order[jnp.where(places < fixed, places, passed)]].set(jnp.asarray(sizes, jnp.int32))

    sizes = jnp.where(number % 4 == 0, named(heavy_load, number // 4), named(ordinary, number - number // 4 - 1))
    mixed = jax.random.permutation(jax.random.fold_in(own, 3), number_of)
    donor, sink = mixed[0:number_of // 2 * 2:2], mixed[1:number_of // 2 * 2:2]
    margin = jnp.minimum(sizes[donor] - 1, reach - sizes[sink]) // 2
    margin = jnp.where((donor == order[0]) | (sink == order[0]) | (sizes[sink] == 0), 0, jnp.maximum(margin, 0))
    passed = jax.random.randint(jax.random.fold_in(own, 4), (number_of // 2,), 0, 1 << 20) % (margin + 1)
    sizes = sizes.at[donor].add(-passed).at[sink].add(passed)
    labels = jnp.searchsorted(jnp.cumsum(sizes), jnp.arange(rows * top), side="right").astype(jnp.int32)
    listing = labels.reshape(top, rows).T
    listing = listing[jax.random.permutation(jax.random.fold_in(own, 1), rows)]
    turn = jax.random.randint(jax.random.fold_in(own, 2), (rows, 1), 0, top)
    return jnp.take_along_axis(listing, (jnp.arange(top)[None, :] + turn) % top, axis=1)


def load_shares(number_of, total, limit, skew, full):
    loads = [(1 << 20) // math.isqrt(rank ** skew) + 1 for rank in range(1, number_of + 1)]
    largest = limit if full else min(limit, max(-(-total // number_of), total * loads[0] // sum(loads)))
    least = 1 if total - largest >= number_of - 1 else 0
    counts, surplus = [largest] + [least] * (number_of - 1), total - largest - least * (number_of - 1)
    while surplus > 0:
        free = [i for i in range(1, number_of) if counts[i] < largest] or [i for i in range(1, number_of) if counts[i] < limit]
        mass, left = sum([loads[i] for i in free]), surplus
        for i in free:
            extra = min(limit - counts[i], max(1, left * loads[i] // mass), surplus)
            counts[i] = counts[i] + extra
            surplus = surplus - extra
    return np.array(counts)


def noise(own_key, extent, scale, reach, cuts=(), kind=jnp.bfloat16):
    entries = scale * jax.random.normal(own_key, extent, jnp.float32)
    if cuts:
        entries = entries * block_scale(own_key, extent, cuts, -0.22, 0.18)
    return jnp.clip(entries, -reach, reach).astype(kind)


def setup_inputs(seed: int = 0) -> dict:
    key_of = jax.random.split(jax.random.key(seed), 14)
    queries = draw_queries(jax.random.fold_in(key_of[13], 71), 0)
    keys = draw_keys(jax.random.fold_in(key_of[13], 71), 0)
    values = noise(key_of[2], (SEQ, KV_HEADS * HEAD_DIM), 1.0, 6.0, ((0, 16), (1, 16)))
    doc_ids = jnp.searchsorted(jnp.cumsum(ragged_sizes(key_of[3], DOCS, SEQ, 3 * TOK_SP, 1)), jnp.arange(SEQ), side="right").astype(jnp.int32)
    sink_logits = jnp.clip(3.0 + 3.0 * jax.random.uniform(key_of[4], (HEADS,), jnp.float32) ** block_scale(key_of[4], (HEADS,), ((0, 16),), -0.2, 0.2), 3.0, 6.0)
    out_weight = noise(key_of[5], (HEADS * HEAD_DIM, D), HEAD_DIM ** -0.5, 0.75, ((0, 16),))
    residual = noise(key_of[6], (SEQ, D), 1.0, 6.0, ((0, 256),))
    norm_gain = jnp.clip(1.0 + 0.18 * jax.random.normal(key_of[7], (D,), jnp.float32), 0.1, 1.9)
    routes_keys = jax.random.split(jax.random.fold_in(key_of[8], 1), SEQ // TOK_DEV)
    routes_turns = jax.random.permutation(jax.random.fold_in(key_of[8], 3), SEQ // TOK_DEV)
    routes = jax.vmap(lambda own, number: deal_out(jax.random.fold_in(key_of[8], 2), own, number, TOK_DEV, EXPERTS, TOP_K, CAP, 2))(routes_keys, routes_turns).reshape((SEQ, TOP_K))
    route_weights = jnp.clip(0.2 + 0.8 * jax.random.uniform(key_of[9], (SEQ, TOP_K), jnp.float32) ** block_scale(key_of[9], (SEQ, TOP_K), ((0, 256),), -0.2, 0.2), 0.2, 1.0)
    gate_weight = noise(key_of[10], (EXPERTS, D, FF), D ** -0.5, 0.125, ((0, 16), (2, 16)))
    up_weight = noise(key_of[11], (EXPERTS, D, FF), D ** -0.5, 0.125, ((0, 16), (2, 16)))
    down_weight = noise(key_of[12], (EXPERTS, FF, D), FF ** -0.5, 0.0625, ((0, 16), (1, 16)))
    return dict(queries=queries, keys=keys, values=values, doc_ids=doc_ids, sink_logits=sink_logits, out_weight=out_weight, residual=residual, norm_gain=norm_gain, routes=routes, route_weights=route_weights, gate_weight=gate_weight, up_weight=up_weight, down_weight=down_weight)


layer_epsilon = 1e-05
masked_score = -1e+30

def reference(queries, keys, values, doc_ids, sink_logits, out_weight, residual, norm_gain, routes, route_weights, gate_weight, up_weight, down_weight):
    reach_back = WINDOW - 1
    group_ratio = HEADS // KV_HEADS
    block_rows = min(512, TOK_SP)
    score_scale = 1.0 / math.sqrt(HEAD_DIM)
    kv_width = KV_HEADS * HEAD_DIM
    padded_keys = jnp.concatenate([jnp.zeros((reach_back, kv_width), keys.dtype), keys], axis=0)
    padded_values = jnp.concatenate([jnp.zeros((reach_back, kv_width), values.dtype), values], axis=0)
    padded_docs = jnp.concatenate([jnp.full((reach_back,), -1, jnp.int32), doc_ids.astype(jnp.int32)], axis=0)
    sink_table = sink_logits.astype(jnp.float32).reshape(KV_HEADS, group_ratio, 1)

    def attend_block(block_index):
        first_row = (block_index * block_rows).astype(jnp.int32)
        query_rows = lax.dynamic_slice_in_dim(queries, first_row, block_rows, 0).astype(jnp.float32)
        query_rows = query_rows.reshape(block_rows, KV_HEADS, group_ratio, HEAD_DIM)
        key_rows = lax.dynamic_slice_in_dim(padded_keys, first_row, block_rows + reach_back, 0).astype(jnp.float32)
        key_rows = key_rows.reshape(block_rows + reach_back, KV_HEADS, HEAD_DIM)
        value_rows = lax.dynamic_slice_in_dim(padded_values, first_row, block_rows + reach_back, 0).astype(jnp.float32)
        value_rows = value_rows.reshape(block_rows + reach_back, KV_HEADS, HEAD_DIM)
        query_docs = lax.dynamic_slice_in_dim(doc_ids.astype(jnp.int32), first_row, block_rows, 0)
        key_docs = lax.dynamic_slice_in_dim(padded_docs, first_row, block_rows + reach_back, 0)
        scores = jnp.einsum('bgrd,sgd->grbs', query_rows, key_rows) * score_scale
        offsets = jnp.arange(block_rows)[:, None] + reach_back - jnp.arange(block_rows + reach_back)[None, :]
        allowed = (offsets >= 0) & (offsets <= reach_back) & (query_docs[:, None] == key_docs[None, :])
        scores = jnp.where(allowed, scores, masked_score)
        row_max = jnp.maximum(scores.max(-1), sink_table)
        exp_scores = jnp.exp(scores - row_max[..., None])
        denominator = exp_scores.sum(-1) + jnp.exp(sink_table - row_max)
        probabilities = lax.optimization_barrier(exp_scores.astype(jnp.bfloat16)).astype(jnp.float32)
        weighted = jnp.einsum('grbs,sgd->bgrd', probabilities, value_rows)
        weighted = weighted / jnp.transpose(denominator, (2, 0, 1))[..., None]
        return weighted.astype(jnp.bfloat16).reshape(block_rows, HEADS * HEAD_DIM)
    attended = lax.map(attend_block, jnp.arange(SEQ // block_rows, dtype=jnp.int32)).reshape(SEQ, HEADS * HEAD_DIM)
    projected = jnp.dot(attended, out_weight, preferred_element_type=jnp.float32)
    stream = residual.astype(jnp.float32) + projected
    mean_value = stream.mean(-1, keepdims=True)
    centred = stream - mean_value
    variance = (centred * centred).mean(-1, keepdims=True)
    normed = (centred * lax.rsqrt(variance + layer_epsilon) * norm_gain.astype(jnp.float32)).astype(jnp.bfloat16)
    blocks_total = SEQ // TOK_DEV
    flat_routes = routes.astype(jnp.int32).reshape(blocks_total, TOP_K * TOK_DEV)
    one_hot = (flat_routes[..., None] == jnp.arange(EXPERTS, dtype=jnp.int32)).astype(jnp.int32)
    slot_ids = lax.optimization_barrier(jnp.sum((jnp.cumsum(one_hot, axis=1) - 1) * one_hot, axis=-1))
    block_base = jnp.arange(blocks_total, dtype=jnp.int32)[:, None] * CAP
    destination = (flat_routes * (blocks_total * CAP) + block_base + slot_ids).reshape(-1).astype(jnp.int32)
    token_index = (jnp.arange(SEQ * TOP_K, dtype=jnp.int32) // TOP_K).astype(jnp.int32)
    buffer_rows = jnp.zeros((EXPERTS * blocks_total * CAP, D), jnp.bfloat16).at[destination].set(normed[token_index])

    def run_expert(expert_index):
        rows_in = lax.dynamic_slice_in_dim(buffer_rows, (expert_index * blocks_total * CAP).astype(jnp.int32), blocks_total * CAP, 0)
        gate = jnp.dot(rows_in, gate_weight[expert_index], preferred_element_type=jnp.float32)
        upward = jnp.dot(rows_in, up_weight[expert_index], preferred_element_type=jnp.float32)
        hidden = (jax.nn.silu(gate) * upward).astype(jnp.bfloat16)
        grouped = hidden.reshape(blocks_total * CAP, N_TP, FF // N_TP).astype(jnp.float32)
        down_groups = down_weight[expert_index].reshape(N_TP, FF // N_TP, D).astype(jnp.float32)
        partials = jnp.einsum('rtf,tfd->trd', grouped, down_groups)
        rounded = lax.optimization_barrier(partials.astype(jnp.bfloat16)).astype(jnp.float32)
        return rounded.sum(0).astype(jnp.bfloat16)
    results = lax.map(run_expert, jnp.arange(EXPERTS, dtype=jnp.int32)).reshape(EXPERTS * blocks_total * CAP, D)
    picked = results[destination].astype(jnp.float32).reshape(SEQ, TOP_K, D)
    combined = lax.optimization_barrier(jnp.sum(picked * route_weights.astype(jnp.float32)[..., None], axis=1))
    return (stream + combined).astype(jnp.bfloat16)
```

```python
import functools
import math

import jax
import jax.numpy as jnp
from jax import lax
from jax.experimental import pallas as pl
from jax.experimental.pallas import tpu as pltpu
from jax.sharding import PartitionSpec as P

HEAD_DIM = 64
WINDOW = 128
ROWS = 144
HALF = 1024
MESH = pl.DeviceIdType.MESH


layer_epsilon = 1e-05
masked_score = -1e30


def passed_along(value, axis, steps):
    count = lax.axis_size(axis)
    first, last = (max(0, -steps), min(count, count - steps))
    return lax.ppermute(value, axis, [(source, source + steps) for source in range(first, last)])


RS_SLOTS = ((3, 1), (4, 0), (2, 1), (3, 0), (1, 1), (2, 0), (1, 0))
RS_NEEDS = (None, None, 0, 1, 2, 3, 5)


def expert_kernel(
    arrived,
    gate,
    up,
    down,
    out,
    rows,
    partial,
    partner_partial,
    sum_up,
    sum_down,
    got_up,
    got_down,
    gate_v,
    up_v,
    down_v,
    load_sem,
    ag_send,
    ag_recv,
    share_send,
    share_recv,
    rs_send,
    rs_recv,
    part_send,
    part_recv,
):
    me = lax.axis_index("tp")
    chip = me // 2
    core = lax.rem(me, 2)
    above, below = lax.rem(me + 2, 16), lax.rem(me + 14, 16)
    partner = me + 1 - 2 * core

    def block(offset):
        return lax.rem(chip + offset + 8, 8)

    loads = [
        pltpu.make_async_copy(arrived, rows.at[chip, core], load_sem.at[0]),
        pltpu.make_async_copy(gate, gate_v, load_sem.at[1]),
        pltpu.make_async_copy(up, up_v, load_sem.at[2]),
        pltpu.make_async_copy(down, down_v, load_sem.at[3]),
    ]
    for load in loads:
        load.start()

    barrier = pltpu.get_barrier_semaphore()
    for other in (above, below, partner):
        pl.semaphore_signal(barrier, inc=1, device_id={"tp": other}, device_id_type=MESH)
    pl.semaphore_wait(barrier, 3)

    def piece(origin_offset, half):
        return rows.at[block(origin_offset), core, :, pl.ds(pl.multiple_of(half * HALF, HALF), HALF)]

    def gather(direction, s, sending):
        distance = s // 2 + 1
        travelled = distance - 1 if sending else distance
        if direction == 0:
            ref = piece(-travelled, lax.rem(s, 2))
        else:
            ref = piece(travelled, 1 - lax.rem(s, 2))
        return pltpu.make_async_remote_copy(
            src_ref=ref,
            dst_ref=ref,
            send_sem=ag_send.at[direction, s],
            recv_sem=ag_recv.at[direction, s],
            device_id={"tp": above if direction == 0 else below},
            device_id_type=MESH,
        )

    def share(direction, s, receiving):
        distance = s // 2 + 1
        offset = -distance if direction == 0 else distance
        half = lax.rem(s, 2) if direction == 0 else 1 - lax.rem(s, 2)
        owner = 1 - core if receiving else core
        ref = rows.at[block(offset), owner, :, pl.ds(pl.multiple_of(half * HALF, HALF), HALF)]
        return pltpu.make_async_remote_copy(
            src_ref=ref,
            dst_ref=ref,
            send_sem=share_send.at[direction, s],
            recv_sem=share_recv.at[direction, s],
            device_id={"tp": partner},
            device_id_type=MESH,
        )

    def share_own(receiving):
        ref = rows.at[chip, 1 - core if receiving else core]
        return pltpu.make_async_remote_copy(
            src_ref=ref,
            dst_ref=ref,
            send_sem=share_send.at[0, 7],
            recv_sem=share_recv.at[0, 7],
            device_id={"tp": partner},
            device_id_type=MESH,
        )

    def share_partial(s, offset):
        b = block(offset)
        return pltpu.make_async_remote_copy(
            src_ref=partial.at[b, 1 - core],
            dst_ref=partner_partial.at[b],
            send_sem=part_send.at[s],
            recv_sem=part_recv.at[s],
            device_id={"tp": partner},
            device_id_type=MESH,
        )

    def reduce_copy(direction, i):
        source, target = (sum_up, got_up) if direction == 0 else (sum_down, got_down)
        return pltpu.make_async_remote_copy(
            src_ref=source.at[i],
            dst_ref=target.at[i],
            send_sem=rs_send.at[direction, i],
            recv_sem=rs_recv.at[direction, i],
            device_id={"tp": above if direction == 0 else below},
            device_id_type=MESH,
        )

    def reduce_step(direction, i):
        distance, half = RS_SLOTS[i]
        if direction == 1:
            distance, half = -distance, 1 - half
        b = block(distance)
        need = RS_NEEDS[i]
        destination, received = (sum_up, got_up) if direction == 0 else (sum_down, got_down)
        if need is not None:
            reduce_copy(direction, need).wait_recv()

        def add(r, _):
            span = pl.ds(pl.multiple_of(r * 16, 16), 16)
            total = partial[b, core, span, half * HALF : (half + 1) * HALF].astype(jnp.float32)
            total += partner_partial[b, span, half * HALF : (half + 1) * HALF].astype(jnp.float32)
            if need is not None:
                total += received[need, span, :].astype(jnp.float32)
            destination[i, span, :] = total.astype(jnp.bfloat16)
            return 0

        lax.fori_loop(0, ROWS // 16, add, 0)
        reduce_copy(direction, i).start()

    loads[0].wait()
    for s in (0, 1):
        for direction in (0, 1):
            gather(direction, s, True).start()
    share_own(False).start()
    for load in loads[1:]:
        load.wait()

    def offset_of(s):
        return jnp.where(lax.rem(s, 2) == 0, s // 2, -((s + 1) // 2))

    def step(s, _):
        @pl.when(s < 7)
        def _():
            for direction in (0, 1):
                gather(direction, s, False).wait_recv()

                @pl.when(s + 2 < 7)
                def _():
                    gather(direction, s + 2, True).start()

                share(direction, s, False).start()

        @pl.when(s == 0)
        def _():
            share_own(True).wait_recv()

        @pl.when(s < 7)
        def _():
            share(0, s, True).wait_recv()

        @pl.when(s > 0)
        def _():
            share(1, s - 1, True).wait_recv()

        @pl.when(s == 7)
        def _():
            share_partial(6, 3).wait_recv()
            share_partial(5, -3).wait_recv()
            reduce_step(0, 0)
            reduce_step(1, 0)

        b = block(offset_of(s))
        x = rows[b].reshape(2 * ROWS, 2 * HALF)
        g = jnp.dot(x, gate_v[...], preferred_element_type=jnp.float32)
        u = jnp.dot(x, up_v[...], preferred_element_type=jnp.float32)
        hidden = (g / (1.0 + jnp.exp(-g)) * u).astype(jnp.bfloat16)
        for n in range(4):
            y = jnp.dot(hidden, down_v[:, n * 512 : (n + 1) * 512], preferred_element_type=jnp.float32)
            partial[b, :, :, n * 512 : (n + 1) * 512] = y.astype(jnp.bfloat16).reshape(2, ROWS, 512)
        share_partial(s, offset_of(s)).start()
        return 0

    lax.fori_loop(0, 8, step, 0)

    for i in range(1, 7):
        if i == 1:
            share_partial(7, -4).wait_recv()
        if i == 2:
            share_partial(4, 2).wait_recv()
            share_partial(3, -2).wait_recv()
        if i == 4:
            share_partial(2, 1).wait_recv()
            share_partial(1, -1).wait_recv()
        reduce_step(0, i)
        reduce_step(1, i)

    share_partial(0, 0).wait_recv()
    for direction in (0, 1):
        for i in (4, 6):
            reduce_copy(direction, i).wait_recv()
    for half, (u_slot, d_slot) in enumerate(((6, 4), (4, 6))):
        def finish(r, _):
            span = pl.ds(pl.multiple_of(r * 16, 16), 16)
            columns = slice(half * HALF, (half + 1) * HALF)
            total = partial[chip, core, span, columns].astype(jnp.float32)
            total += partner_partial[chip, span, columns].astype(jnp.float32)
            total += got_up[u_slot, span, :].astype(jnp.float32)
            total += got_down[d_slot, span, :].astype(jnp.float32)
            out[span, columns] = total.astype(jnp.bfloat16)
            return 0

        lax.fori_loop(0, ROWS // 16, finish, 0)

    share_own(False).wait_send()
    for s in range(7):
        for direction in (0, 1):
            gather(direction, s, True).wait_send()
            share(direction, s, False).wait_send()
            reduce_copy(direction, s).wait_send()
    for s in range(8):
        share_partial(s, s // 2 if s % 2 == 0 else -((s + 1) // 2)).wait_send()


def experts(arrived, gate, up, down):
    any_space = pl.BlockSpec(memory_space=pltpu.HBM)
    bf16 = jnp.bfloat16
    return pl.pallas_call(
        expert_kernel,
        out_shape=jax.ShapeDtypeStruct((ROWS, 2 * HALF), bf16),
        in_specs=[any_space] * 4,
        out_specs=pl.BlockSpec(memory_space=pltpu.VMEM),
        scratch_shapes=[
            pltpu.VMEM((8, 2, ROWS, 2 * HALF), bf16),
            pltpu.VMEM((8, 2, ROWS, 2 * HALF), bf16),
            pltpu.VMEM((8, ROWS, 2 * HALF), bf16),
            pltpu.VMEM((7, ROWS, HALF), bf16),
            pltpu.VMEM((7, ROWS, HALF), bf16),
            pltpu.VMEM((7, ROWS, HALF), bf16),
            pltpu.VMEM((7, ROWS, HALF), bf16),
            pltpu.VMEM(gate.shape, bf16),
            pltpu.VMEM(up.shape, bf16),
            pltpu.VMEM(down.shape, bf16),
            pltpu.SemaphoreType.DMA((4,)),
            pltpu.SemaphoreType.DMA((2, 7)),
            pltpu.SemaphoreType.DMA((2, 7)),
            pltpu.SemaphoreType.DMA((2, 8)),
            pltpu.SemaphoreType.DMA((2, 8)),
            pltpu.SemaphoreType.DMA((2, 7)),
            pltpu.SemaphoreType.DMA((2, 7)),
            pltpu.SemaphoreType.DMA((8,)),
            pltpu.SemaphoreType.DMA((8,)),
        ],
        compiler_params=pltpu.CompilerParams(
            collective_id=1, has_side_effects=True, vmem_limit_bytes=56 * 1024 * 1024
        ),
        cost_estimate=pl.CostEstimate(
            flops=2 * 2304 * 2048 * 448 * 3, bytes_accessed=8 << 20, transcendentals=2304 * 448
        ),
        name="experts",
    )(arrived, gate, up, down)


def local(
    queries,
    keys,
    values,
    doc_ids,
    sink_logits,
    out_weight,
    residual,
    norm_gain,
    routes,
    route_weights,
    gate_weight,
    up_weight,
    down_weight,
):
    span_rows = queries.shape[0]
    kv_width = keys.shape[1]
    kv_groups = kv_width // HEAD_DIM
    heads_here = queries.shape[1] // HEAD_DIM
    group_ratio = heads_here // kv_groups
    reach_back = WINDOW - 1
    score_scale = 1.0 / math.sqrt(HEAD_DIM)
    doc_float = (doc_ids + 1).astype(jnp.float32)
    key_value = jnp.concatenate([keys, values], axis=1).astype(jnp.float32)
    tail_pairs, tail_docs = (
        passed_along(key_value[span_rows - reach_back :].astype(jnp.bfloat16), "sp", 1).astype(
            jnp.float32
        ),
        passed_along(doc_float[span_rows - reach_back :].astype(jnp.bfloat16), "sp", 1).astype(
            jnp.float32
        ),
    )
    all_keys = jnp.concatenate([tail_pairs[:, :kv_width].astype(jnp.bfloat16), keys], axis=0)
    all_values = jnp.concatenate([tail_pairs[:, kv_width:].astype(jnp.bfloat16), values], axis=0)
    all_docs = jnp.concatenate([tail_docs, doc_float], axis=0)
    block_rows = min(512, span_rows)
    sink_table = sink_logits.reshape(kv_groups, group_ratio, 1)
    offsets = (
        jnp.arange(block_rows)[:, None] + reach_back - jnp.arange(block_rows + reach_back)[None, :]
    )
    window_mask = (offsets >= 0) & (offsets <= reach_back)
    pieces = []
    for block_index in range(span_rows // block_rows):
        first_row = block_index * block_rows
        query_rows = queries[first_row : first_row + block_rows].reshape(
            block_rows, kv_groups, group_ratio, HEAD_DIM
        )
        key_rows = all_keys[first_row : first_row + block_rows + reach_back].reshape(
            block_rows + reach_back, kv_groups, HEAD_DIM
        )
        value_rows = all_values[first_row : first_row + block_rows + reach_back].reshape(
            block_rows + reach_back, kv_groups, HEAD_DIM
        )
        scores = (
            jnp.einsum("bgrd,sgd->grbs", query_rows, key_rows, preferred_element_type=jnp.float32)
            * score_scale
        )
        same_doc = (
            doc_float[first_row : first_row + block_rows][:, None]
            == all_docs[first_row : first_row + block_rows + reach_back][None, :]
        )
        scores = jnp.where(window_mask & same_doc, scores, masked_score)
        row_max = jnp.maximum(scores.max(-1), sink_table)
        exp_scores = jnp.exp(scores - row_max[..., None])
        denominator = exp_scores.sum(-1) + jnp.exp(sink_table - row_max)
        weighted = jnp.einsum(
            "grbs,sgd->bgrd",
            exp_scores.astype(jnp.bfloat16),
            value_rows,
            preferred_element_type=jnp.float32,
        )
        weighted = weighted / jnp.transpose(denominator, (2, 0, 1))[..., None]
        pieces.append(weighted.astype(jnp.bfloat16).reshape(block_rows, heads_here * HEAD_DIM))
    attended = jnp.concatenate(pieces, axis=0)
    token_major = lax.all_to_all(attended, "tp", split_axis=0, concat_axis=1, tiled=True)
    projected = jnp.dot(
        token_major,
        lax.all_gather(out_weight, "tp", axis=0, tiled=True),
        preferred_element_type=jnp.float32,
    )
    stream = residual.astype(jnp.float32) + projected
    mean_value = stream.mean(-1, keepdims=True)
    centred = stream - mean_value
    variance = (centred * centred).mean(-1, keepdims=True)
    normed = (centred * lax.rsqrt(variance + layer_epsilon) * norm_gain).astype(jnp.bfloat16)
    token_count = residual.shape[0]
    width = residual.shape[1]
    route_count = routes.shape[1]
    expert_count = lax.axis_size("sp") * gate_weight.shape[0]
    capacity = 9 * route_count * token_count // (8 * expert_count)
    flat_routes = routes.reshape(-1)
    one_hot = (flat_routes[:, None] == jnp.arange(expert_count)[None, :]).astype(jnp.int32)
    slot_ids = jnp.sum((jnp.cumsum(one_hot, axis=0) - 1) * one_hot, axis=1)
    destination = flat_routes * capacity + slot_ids
    slot_range = jnp.arange(expert_count * capacity)
    selector = jnp.any(
        slot_range[:, None, None] == destination.reshape(token_count, route_count)[None], axis=2
    )
    dispatch = jnp.dot(
        selector.astype(jnp.bfloat16), normed, preferred_element_type=jnp.float32
    ).astype(jnp.bfloat16)
    inbound = lax.all_to_all(
        dispatch.reshape(expert_count, capacity, width),
        "sp",
        split_axis=0,
        concat_axis=0,
        tiled=True,
    )
    arrived = inbound.reshape(-1, width)
    returned = experts(arrived, gate_weight[0], up_weight[0], down_weight[0])
    back_rows = lax.all_to_all(
        returned.reshape(inbound.shape), "sp", split_axis=0, concat_axis=0, tiled=True
    ).reshape(-1, width)
    picked = back_rows[destination].astype(jnp.float32).reshape(token_count, route_count, width)
    combined = jnp.sum(picked * route_weights[..., None], axis=1)
    return (stream + combined).astype(jnp.bfloat16)


def solution(mesh):
    placed = (
        P("sp", "tp"),
        P("sp", "tp"),
        P("sp", "tp"),
        P("sp"),
        P("tp"),
        P("tp", None),
        P(("sp", "tp"), None),
        P(),
        P(("sp", "tp"), None),
        P(("sp", "tp"), None),
        P("sp", None, "tp"),
        P("sp", None, "tp"),
        P("sp", "tp", None),
    )
    return jax.shard_map(
        local, mesh=mesh, in_specs=placed, out_specs=P(("sp", "tp"), None), check_vma=False
    )
```
